512 devices in a mesh: ep: 16 (over y, x), tp: 32 (over z, core).
Axes of the slice: x: 4, y: 4, z: 16, core: 2. Of those that a mesh axis runs over, the one named last changes fastest.
Arguments:
- features: bfloat16 [256, 1024], P('ep', 'tp'), may hold values from -6 to 6
- key_table: bfloat16 [262144, 1024], P('ep', 'tp'), may hold values from -0.1875 to 0.1875
- value_table: bfloat16 [262144, 1024], P('ep', 'tp'), may hold values from -6 to 6
- chosen: int32 [256, 4, 16], P('ep'), may hold values from 0 to 262143
- scores: float32 [256, 4, 16], P('ep'), may hold values from -8 to 8
Outputs:
- mixed: bfloat16 [256, 1024], P('ep', 'tp')
The draws below stay inside these ranges and needn't reach their ends.
Inputs may be any that keep to these rules, and one draw needn't show every extreme that they name: Every chosen row is a row of the tables, 0 to 262143; rows may repeat, and a few rows are far more popular than the rest.
All inputs are finite; a program needn't handle non-finite values.
Results may differ from the reference program's by a relative error of at most 0.0065.
Values may be sent and summed in bfloat16 or wider, within the bound.
A program may use at most 64 MiB of HBM per device.

```python
import math
import jax
import jax.numpy as jnp
import numpy as np
from jax import lax

D = 1024
HEADS = 4
TOPK = 16
TOK_DEV = 16
TOKENS = 256
EXPERTS = 262144


def plant(result, rng, low, largest):
    index_at = [jax.random.randint(jax.random.fold_in(rng, axis), (), 0, length) for axis, length in enumerate(result.shape)]
    main_axis = result.shape.index(max(result.shape))
    neighbour = index_at[:main_axis] + [(index_at[main_axis] + 1) % result.shape[main_axis]] + index_at[main_axis + 1:]
    return result.at[tuple(index_at)].set(low).at[tuple(neighbour)].set(largest)


def shard_levels(key, extent, cuts, least, top_value):
    def one(dim, shards_of):
        steps = jax.random.uniform(jax.random.fold_in(jax.random.fold_in(key, 6), dim), (shards_of,), jnp.float32, least / len(cuts), top_value / len(cuts))
        return jnp.repeat(jnp.exp(steps), extent[dim] // shards_of).reshape((-1,) + (1,) * (len(extent) - dim - 1))

    level = one(*cuts[0])
    for cut in cuts[1:]:
        level = level * one(*cut)
    return level


def ranked_wide(own_key, shape, number_of, lean):
    loads = [min(1 << octave, number_of + 1 - (1 << octave)) * (1 << 20) // math.isqrt((1 << octave) ** lean) + 1 for octave in range((number_of + 1).bit_length()) if 1 << octave <= number_of]
    scale = 1 + sum(loads) // (1 << 30)
    listing = np.cumsum(np.array([max(1, weight // scale) for weight in loads]))
    lot = jax.random.randint(jax.random.fold_in(own_key, 1), shape, 0, int(listing[len(loads) - 1]))
    start = jnp.left_shift(1, jnp.searchsorted(jnp.asarray(listing, jnp.int32), lot, side="right").astype(jnp.int32))
    grade = start - 1 + jax.random.randint(jax.random.fold_in(own_key, 4), shape, 0, 1 << 30) % jnp.minimum(start, number_of + 1 - start)
    return jax.random.permutation(jax.random.fold_in(own_key, 2), number_of)[grade].astype(jnp.int32)


def scatter_about(own_key, dims, width, limit, split=(), dtype=jnp.bfloat16):
    entries = jax.random.normal(own_key, dims, jnp.float32) * width
    if len(split) > 0:
        entries = shard_levels(own_key, dims, split, -0.22, 0.18) * entries
    return jnp.clip(entries, min=-limit, max=limit).astype(dtype)


def setup_inputs(seed: int = 0) -> dict:
    seeds = jax.random.split(jax.random.key(seed), 6)
    return {
        "features": scatter_about(seeds[0], (TOKENS, D), 1.0, 6.0, ((0, 16), (1, 32))),
        "key_table": scatter_about(seeds[1], (EXPERTS, D), D ** -0.5, 0.1875, ((0, 16), (1, 32))),
        "value_table": scatter_about(seeds[2], (EXPERTS, D), 1.0, 6.0, ((0, 16), (1, 32))),
        "chosen": plant(ranked_wide(seeds[3], (TOKENS, HEADS, TOPK), EXPERTS, 2), jax.random.fold_in(seeds[3], 3), 0, EXPERTS - 1).astype(jnp.int32),
        "scores": scatter_about(seeds[4], (TOKENS, HEADS, TOPK), 2.0, 8.0, ((0, 16),), jnp.float32),
    }


def reference(features, key_table, value_table, chosen, scores):
    gate_weights = jax.nn.softmax(scores, axis=-1)
    block_count = TOKENS // TOK_DEV

    def per_block(block_data):
        block_tokens, block_rows, block_gates = block_data
        flat_rows = block_rows.reshape(-1).astype(jnp.int32)
        key_rows = jnp.take(key_table, flat_rows, axis=0).reshape(TOK_DEV, HEADS * TOPK, D).astype(jnp.float32)
        products = jnp.einsum("tjd,td->tj", key_rows, block_tokens.astype(jnp.float32), precision=lax.Precision.HIGHEST)
        row_weights = (block_gates.reshape(TOK_DEV, HEADS * TOPK) * jax.nn.gelu(products, approximate=False)).astype(jnp.bfloat16)
        value_rows = jnp.take(value_table, flat_rows, axis=0).reshape(TOK_DEV, HEADS * TOPK, D).astype(jnp.float32)
        summed = jnp.einsum("tj,tjd->td", row_weights.astype(jnp.float32), value_rows, precision=lax.Precision.HIGHEST)
        return summed.astype(jnp.bfloat16)

    outputs = lax.map(per_block, (features.reshape(block_count, TOK_DEV, D),
                                  chosen.reshape(block_count, TOK_DEV, HEADS, TOPK),
                                  gate_weights.reshape(block_count, TOK_DEV, HEADS, TOPK)))
    return outputs.reshape(TOKENS, D)
```

```python
import functools

import jax
import jax.numpy as jnp
from jax import lax
from jax.experimental import pallas as pl
from jax.experimental.pallas import tpu as pltpu
from jax.sharding import PartitionSpec as P

MESH = pl.DeviceIdType.MESH
F32 = jnp.float32
BF16 = jnp.bfloat16
I32 = jnp.int32


NEAR = sorted((d for d in range(1, 16)), key=lambda d: min(d // 4, 4 - d // 4) + min(d % 4, 4 - d % 4))
FAR = NEAR[::-1]
RING = sorted(range(1, 16), key=lambda d: -min(d, 16 - d))


def other(ep, d):
    y, x = lax.div(ep, 4), lax.rem(ep, 4)
    return lax.rem(y + d // 4, 4) * 4 + lax.rem(x + d % 4, 4)


def iota(shape, dim):
    return lax.broadcasted_iota(I32, shape, dim)


def one(cond):
    return jnp.where(cond, 1.0, 0.0).astype(BF16)


def mm(a, b):
    return jnp.dot(a, b, preferred_element_type=F32)


def gelu(x):
    return 0.5 * x * (1.0 + lax.erf(x * (2.0 ** -0.5)))


def compact(ch, sc, cap):
    nb = cap // 128
    na = 16 * nb
    own = lax.shift_right_logical(ch, 14)
    row = ch & 16383
    rep = one((iota((16, 256), 1) & 15) == iota((16, 256), 0))
    ownrep = mm(own.astype(F32).astype(BF16), rep)
    hit = ownrep == lax.shift_right_logical(iota((64, 256), 1), 4).astype(F32)
    hits = one(hit)
    before = mm(one(iota((64, 64), 1) < iota((64, 64), 0)), hits)
    total = mm(jnp.ones((8, 64), BF16), hits)
    r2, c2 = iota((256, 256), 0), iota((256, 256), 1)
    step = one((lax.shift_right_logical(r2, 4) == lax.shift_right_logical(c2, 4)) & ((r2 & 15) < (c2 & 15)))
    start = mm(total.astype(BF16), step)
    over = jnp.max(jnp.where(start + total > float(cap), 1.0, 0.0), axis=1, keepdims=True)[0:1]
    place = jnp.where(hit, before + start[0:1], 0.0).astype(I32)
    fold = one((iota((256, 16), 0) & 15) == iota((256, 16), 1))
    low = mm((place & 255).astype(F32).astype(BF16), fold)
    high = mm(lax.shift_right_logical(place, 8).astype(F32).astype(BF16), fold)
    rank = (low + 256.0 * high).astype(I32)
    line = own * nb + lax.shift_right_logical(rank, 7)
    line = jnp.where(rank < cap, line, -1)
    lane = rank & 127
    top = jnp.max(sc, axis=1, keepdims=True)
    ex = jnp.exp(sc - top)
    gate = ex / jnp.sum(ex, axis=1, keepdims=True)
    wide = jnp.concatenate(
        [line.astype(F32), row.astype(F32), gate, jnp.zeros((64, 80), F32)], axis=1)
    wide = jnp.concatenate([wide, jnp.zeros((64, 128), F32)], axis=0)
    turned = wide.T

    def two(x):
        return jnp.concatenate([x[0:8, 0:64], x[8:16, 0:64]], axis=1)

    line_t = two(turned[0:16]).astype(I32)
    row_t = two(turned[16:32]).astype(I32)
    gate_t = two(turned[32:48])
    g1 = gate_t.astype(BF16).astype(F32)
    g2 = (gate_t - g1).astype(BF16).astype(F32)
    g3 = gate_t - g1 - g2
    token = lax.shift_right_logical(iota((8, 128), 1) & 63, 2)
    pieces = (
        (row_t & 255).astype(F32),
        (lax.shift_right_logical(row_t, 8) & 31).astype(F32),
        (lax.shift_right_logical(row_t, 13) * 16 + token).astype(F32),
        g1, g2, g3,
    )
    lane2 = jnp.concatenate([lane[:, 0:8], lane[:, 8:16]], axis=0)
    lefts, rights = [], []
    for k in range(8):
        at = iota((na, 128), 0) == line_t[k : k + 1]
        lefts.append(jnp.concatenate([jnp.where(at, p[k : k + 1], 0.0) for p in pieces], axis=0).astype(BF16))
        rights.append(one(iota((128, 128), 1) == lane2[:, k : k + 1]))
    got = mm(jnp.concatenate(lefts, axis=1), jnp.concatenate(rights, axis=0))
    rows = got[0:na] + 256.0 * got[na : 2 * na]
    sels = got[2 * na : 3 * na]
    gates = got[3 * na : 4 * na] + got[4 * na : 5 * na] + got[5 * na : 6 * na]
    return rows, sels, gates, over


def kernel(cap, feat, key_hbm, val_hbm, chosen_hbm, scores_hbm, out, flag,
           chosen, scores, keys, vals, table, msg, got, feats, fplace, idx_v, idx_s, sel_v, gate_v, picked,
           part, pair, half, zbuf, wbuf, wvec, obuf, dbuf,
           in_sem, idx_sem, a_send, a_recv, f_send, f_recv, p_send, p_recv, z_send, z_recv, w_send, w_recv, d_send, d_recv):
    nb = cap // 128
    nq = 16 * nb
    nh = nq // 2
    ep, tp = lax.axis_index("ep"), lax.axis_index("tp")
    core, z = lax.rem(tp, 2), lax.div(tp, 2)
    mate = tp + 1 - 2 * core

    ins = [pltpu.make_async_copy(a, b, in_sem.at[k]) for k, (a, b) in enumerate(
        ((chosen_hbm, chosen), (scores_hbm, scores), (key_hbm, keys), (val_hbm, vals)))]
    for c in ins:
        c.start()

    barrier = pltpu.get_barrier_semaphore()
    for d in RING:
        pl.semaphore_signal(barrier, inc=1, device_id=(ep, lax.rem(tp + 2 * d, 32)), device_id_type=MESH)
    for d in FAR:
        pl.semaphore_signal(barrier, inc=1, device_id=(other(ep, d), tp), device_id_type=MESH)
    pl.semaphore_signal(barrier, inc=1, device_id=(ep, mate), device_id_type=MESH)

    ins[0].wait()
    ins[1].wait()
    rows, sels, gates, over = compact(chosen[...], scores[...], cap)
    for e in range(16):
        msg[e, 0:nb] = rows[e * nb : (e + 1) * nb]
        msg[e, nb : 2 * nb] = sels[e * nb : (e + 1) * nb]
        msg[e, 2 * nb : 3 * nb] = gates[e * nb : (e + 1) * nb]
        msg[e, 3 * nb : 3 * nb + 1] = jnp.broadcast_to(over, (1, 128))

    def list_copy(d):
        e = other(ep, d)
        return pltpu.make_async_remote_copy(
            src_ref=msg.at[e], dst_ref=got.at[ep], send_sem=a_send.at[d], recv_sem=a_recv.at[d],
            device_id=(e, tp), device_id_type=MESH)

    def feat_copy(d):
        e = other(ep, d)
        return pltpu.make_async_remote_copy(
            src_ref=feat, dst_ref=feats.at[ep], send_sem=f_send.at[d], recv_sem=f_recv.at[d],
            device_id=(e, tp), device_id_type=MESH)

    pl.semaphore_wait(barrier, 31)
    for d in FAR:
        list_copy(d).start()
    for d in FAR:
        feat_copy(d).start()
    got[ep] = msg[ep]
    feats[ep] = feat[...]
    ins[2].wait()
    ins[3].wait()

    def turn(b, _):
        at = pl.multiple_of(b * 128, 128)
        block = jnp.concatenate(
            [keys[:, pl.ds(at, 128)], vals[:, pl.ds(at, 128)],
             keys[:, pl.ds(at + 8192, 128)], vals[:, pl.ds(at + 8192, 128)]], axis=0).astype(F32)
        table[pl.ds(at, 128), :] = block.T
        return 0

    lax.fori_loop(0, 64, turn, 0)

    for d in NEAR:
        list_copy(d).wait_recv()
    for s in range(16):
        idx_v[s * nb : (s + 1) * nb] = got[s, 0:nb].astype(I32)

    def idx_copy(q):
        return pltpu.make_async_copy(idx_v.at[q], idx_s.at[pl.ds(q * 128, 128)], idx_sem.at[q])

    worst = got[0, 3 * nb : 3 * nb + 1]
    for s in range(16):
        sel_v[s * nb : (s + 1) * nb] = got[s, nb : 2 * nb].astype(I32)
        gate_v[s * nb : (s + 1) * nb] = got[s, 2 * nb : 3 * nb]
        if s:
            worst = jnp.maximum(worst, got[s, 3 * nb : 3 * nb + 1])
    for q in range(nq):
        idx_copy(q).start()
    for d in NEAR:
        feat_copy(d).wait_recv()
    flag[0, 0] = jnp.max(worst).astype(I32)
    place0 = one(iota((32, 128), 0) == iota((32, 128), 1))
    place1 = one(iota((32, 128), 0) + 64 == iota((32, 128), 1))
    for s in range(16):
        f = feats[s]
        fplace[s, 0:16] = mm(f, place0).astype(BF16)
        fplace[s, 16:32] = mm(f, place1).astype(BF16)
    for q in range(nq):
        idx_copy(q).wait()

    def gather(g, _):
        base = pl.multiple_of(g * 16, 16)
        for j in range(16):
            r = idx_s[base + j] & 8191
            picked[pl.ds(base + j, 1), :] = table[pl.ds(r, 1), :]
        return 0

    lax.fori_loop(0, nq * 8, gather, 0)

    def dots(g, _):
        for j in range(8):
            q = g * 8 + j
            f = fplace[lax.div(q, nb)]
            rows_q = picked[pl.ds(pl.multiple_of(q * 128, 128), 128), :].astype(BF16)
            all_q = lax.dot_general(f, rows_q, (((1,), (1,)), ((), ())), preferred_element_type=F32)
            mine = iota((32, 128), 0) == sel_v[pl.ds(q, 1), :]
            part[pl.ds(q, 1), :] = jnp.sum(jnp.where(mine, all_q, 0.0), axis=0, keepdims=True)
        return 0

    lax.fori_loop(0, nq // 8, dots, 0)

    mine_at = pl.multiple_of(core * nh, 8)
    theirs_at = pl.multiple_of((1 - core) * nh, 8)
    pair_copy = pltpu.make_async_remote_copy(
        src_ref=part.at[pl.ds(theirs_at, nh)], dst_ref=pair, send_sem=p_send, recv_sem=p_recv,
        device_id=(ep, mate), device_id_type=MESH)
    pair_copy.start()
    pair_copy.wait_recv()
    half[...] = (part[pl.ds(mine_at, nh), :] + pair[...]).astype(BF16)

    def z_copy(d):
        return pltpu.make_async_remote_copy(
            src_ref=half, dst_ref=zbuf.at[z], send_sem=z_send.at[d], recv_sem=z_recv.at[d],
            device_id=(ep, lax.rem(tp + 2 * d, 32)), device_id_type=MESH)

    for d in RING:
        z_copy(d).start()
    zbuf[z] = half[...]
    for d in RING:
        z_copy(d).wait_recv()
    whole = zbuf[0].astype(F32)
    for k in range(1, 16):
        whole = whole + zbuf[k].astype(F32)
    wbuf[core] = (gate_v[pl.ds(mine_at, nh), :] * gelu(whole)).astype(BF16)
    w_copy = pltpu.make_async_remote_copy(
        src_ref=wbuf.at[core], dst_ref=wbuf.at[core], send_sem=w_send, recv_sem=w_recv,
        device_id=(ep, mate), device_id_type=MESH)
    w_copy.start()
    w_copy.wait_recv()
    wvec[0:nh] = wbuf[0].astype(F32)
    wvec[nh:nq] = wbuf[1].astype(F32)

    def out_copy(d):
        s = other(ep, d)
        return pltpu.make_async_remote_copy(
            src_ref=obuf.at[s], dst_ref=dbuf.at[ep], send_sem=d_send.at[d], recv_sem=d_recv.at[d],
            device_id=(s, tp), device_id_type=MESH)

    for s in range(16):
        acc = None
        for j in range(nb):
            q = s * nb + j
            mine = iota((32, 128), 0) == sel_v[q : q + 1]
            spread = jnp.where(mine, wvec[q : q + 1], 0.0).astype(BF16)
            term = mm(spread, picked[q * 128 : (q + 1) * 128].astype(BF16))
            acc = term if acc is None else acc + term
        obuf[s] = acc[0:16] + pltpu.roll(acc[16:32], 64, 1)
    for d in FAR:
        out_copy(d).start()
    dbuf[ep] = obuf[ep]
    for d in NEAR:
        out_copy(d).wait_recv()
    full = dbuf[0]
    for k in range(1, 16):
        full = full + dbuf[k]
    out[...] = pltpu.roll(full, 96, 1)[:, 0:32].astype(BF16)

    for d in NEAR:
        list_copy(d).wait_send()
        feat_copy(d).wait_send()
        z_copy(d).wait_send()
        out_copy(d).wait_send()
    pair_copy.wait_send()
    w_copy.wait_send()


def run(cap, cid, feat, key_t, val_t, chosen, scores):
    nb = cap // 128
    nq = 16 * nb
    nh = nq // 2
    mr = (3 * nb + 1 + 7) // 8 * 8
    dma = pltpu.SemaphoreType.DMA
    vmem = pltpu.VMEM
    return pl.pallas_call(
        functools.partial(kernel, cap),
        out_shape=(jax.ShapeDtypeStruct((16, 32), BF16), jax.ShapeDtypeStruct((1, 1), I32)),
        in_specs=[pl.BlockSpec(memory_space=vmem), pl.BlockSpec(memory_space=pl.ANY), pl.BlockSpec(memory_space=pl.ANY),
                  pl.BlockSpec(memory_space=pl.ANY), pl.BlockSpec(memory_space=pl.ANY)],
        out_specs=(pl.BlockSpec(memory_space=vmem), pl.BlockSpec(memory_space=pltpu.SMEM)),
        scratch_shapes=[
            vmem((64, 16), I32), vmem((64, 16), F32), vmem((32, 16384), BF16), vmem((32, 16384), BF16), vmem((8192, 128), F32),
            vmem((16, mr, 128), F32), vmem((16, mr, 128), F32), vmem((16, 16, 32), BF16), vmem((16, 32, 128), BF16),
            vmem((nq, 128), I32), pltpu.SMEM((nq * 128,), I32), vmem((nq, 128), I32), vmem((nq, 128), F32),
            vmem((nq * 128, 128), F32),
            vmem((nq, 128), F32), vmem((nh, 128), F32), vmem((nh, 128), BF16), vmem((16, nh, 128), BF16),
            vmem((2, nh, 128), BF16), vmem((nq, 128), F32), vmem((16, 16, 128), F32), vmem((16, 16, 128), F32),
            dma((4,)), dma((nq,)), dma((16,)), dma((16,)), dma((16,)), dma((16,)), dma, dma, dma((16,)), dma((16,)), dma, dma,
            dma((16,)), dma((16,)),
        ],
        compiler_params=pltpu.CompilerParams(collective_id=cid, has_side_effects=True, vmem_limit_bytes=48 << 20),
    )(feat, key_t, val_t, chosen, scores)


def blocks(func, arrays):
    split = tuple(x.reshape((8, 32) + x.shape[1:]) for x in arrays)
    done = lax.map(func, split)
    return done.reshape((256,) + done.shape[2:])


def dense(features, key_table, value_table, chosen, scores):
    first = lax.axis_index("ep") * 16384
    every = lax.all_gather(chosen, "ep", axis=0, tiled=True)
    gates = lax.all_gather(jax.nn.softmax(scores, axis=-1), "ep", axis=0, tiled=True).reshape(256, 64)
    tokens = lax.all_gather(features, "ep", axis=0, tiled=True)
    shifted = every.reshape(256, 64) - first
    owned = (shifted >= 0) & (shifted < 16384)
    rows = jnp.clip(shifted, 0, 16383)

    def dots(pair):
        block, at = pair
        full = lax.dot_general(block, key_table, (((1,), (1,)), ((), ())), preferred_element_type=F32)
        return jnp.take_along_axis(full, at, axis=1)

    partial = jnp.where(owned, blocks(dots, (tokens, rows)), 0.0)
    products = jnp.concatenate(
        [lax.all_gather(partial[k * 64 : (k + 1) * 64], "tp").sum(0) for k in range(4)], axis=0)
    weights = (gates * jax.nn.gelu(products, approximate=False)).astype(BF16)
    weights = jnp.where(owned, weights, jnp.zeros_like(weights))

    def spread(pair):
        block, at = pair
        ids = lax.broadcasted_iota(I32, at.shape, 0)
        full = jnp.zeros((32, 16384), F32).at[ids, at].add(block.astype(F32))
        upper = full.astype(BF16)
        lower = (full - upper.astype(F32)).astype(BF16)
        return mm(upper, value_table) + mm(lower, value_table)

    terms = lax.all_gather(blocks(spread, (weights, rows)), "ep").sum(0)
    return lax.dynamic_slice_in_dim(terms, lax.axis_index("ep") * 16, 16, 0).astype(BF16)


def local(features, key_table, value_table, chosen, scores):
    quick, flag = run(256, 0, features, key_table.T, value_table.T, chosen.reshape(64, 16), scores.reshape(64, 16))
    return lax.cond(flag[0, 0] > 0, lambda: dense(features, key_table, value_table, chosen, scores), lambda: quick)


def solution(mesh):
    spec = P("ep", "tp")
    whole = P("ep", None, None)
    return jax.shard_map(local, mesh=mesh, in_specs=(spec, spec, spec, whole, whole), out_specs=spec, check_vma=False)
```

```python
import functools

import jax
import jax.numpy as jnp
from jax import lax
from jax.experimental import pallas as pl
from jax.experimental.pallas import tpu as pltpu
from jax.sharding import PartitionSpec as P

MESH = pl.DeviceIdType.MESH
F32 = jnp.float32
BF16 = jnp.bfloat16
I32 = jnp.int32


def hops(d):
    return min(d // 4, 4 - d // 4) + min(d % 4, 4 - d % 4)


ORDER = sorted(range(16), key=hops)
BACK = [(-(d // 4)) % 4 * 4 + (-(d % 4)) % 4 for d in ORDER]
RING = sorted(range(1, 16), key=lambda d: -min(d, 16 - d))


def other(ep, d):
    y, x = lax.div(ep, 4), lax.rem(ep, 4)
    return lax.rem(y + d // 4, 4) * 4 + lax.rem(x + d % 4, 4)


def iota(shape, dim):
    return lax.broadcasted_iota(I32, shape, dim)


def one(cond):
    return jnp.where(cond, 1.0, 0.0).astype(BF16)


def mm(a, b):
    return jnp.dot(a, b, preferred_element_type=F32)


def gelu(x):
    return 0.5 * x * (1.0 + lax.erf(x * (2.0 ** -0.5)))


def compact(ch, sc, cap):
    nb = cap // 128
    na = 16 * nb
    own = lax.shift_right_logical(ch, 14)
    row = ch & 16383
    rep = one((iota((16, 256), 1) & 15) == iota((16, 256), 0))
    ownrep = mm(own.astype(F32).astype(BF16), rep)
    hit = ownrep == lax.shift_right_logical(iota((64, 256), 1), 4).astype(F32)
    hits = one(hit)
    before = mm(one(iota((64, 64), 1) < iota((64, 64), 0)), hits)
    total = mm(jnp.ones((8, 64), BF16), hits)
    r2, c2 = iota((256, 256), 0), iota((256, 256), 1)
    step = one((lax.shift_right_logical(r2, 4) == lax.shift_right_logical(c2, 4)) & ((r2 & 15) < (c2 & 15)))
    start = mm(total.astype(BF16), step)
    over = jnp.max(jnp.where(start + total > float(cap), 1.0, 0.0), axis=1, keepdims=True)[0:1]
    place = jnp.where(hit, before + start[0:1], 0.0).astype(I32)
    fold = one((iota((256, 16), 0) & 15) == iota((256, 16), 1))
    low = mm((place & 255).astype(F32).astype(BF16), fold)
    high = mm(lax.shift_right_logical(place, 8).astype(F32).astype(BF16), fold)
    rank = (low + 256.0 * high).astype(I32)
    line = own * nb + lax.shift_right_logical(rank, 7)
    line = jnp.where(rank < cap, line, -1)
    lane = rank & 127
    top = jnp.max(sc, axis=1, keepdims=True)
    ex = jnp.exp(sc - top)
    gate = ex / jnp.sum(ex, axis=1, keepdims=True)
    wide = jnp.concatenate(
        [line.astype(F32), row.astype(F32), gate, jnp.zeros((64, 80), F32)], axis=1)
    wide = jnp.concatenate([wide, jnp.zeros((64, 128), F32)], axis=0)
    turned = wide.T

    def two(x):
        return jnp.concatenate([x[0:8, 0:64], x[8:16, 0:64]], axis=1)

    line_t = two(turned[0:16]).astype(I32)
    row_t = two(turned[16:32]).astype(I32)
    gate_t = two(turned[32:48])
    g1 = gate_t.astype(BF16).astype(F32)
    g2 = (gate_t - g1).astype(BF16).astype(F32)
    g3 = gate_t - g1 - g2
    token = lax.shift_right_logical(iota((8, 128), 1) & 63, 2)
    pieces = (
        (row_t & 255).astype(F32),
        (lax.shift_right_logical(row_t, 8) & 31).astype(F32),
        (lax.shift_right_logical(row_t, 13) * 16 + token).astype(F32),
        g1, g2, g3,
    )
    lane2 = jnp.concatenate([lane[:, 0:8], lane[:, 8:16]], axis=0)
    lefts, rights = [], []
    for k in range(8):
        at = iota((na, 128), 0) == line_t[k : k + 1]
        lefts.append(jnp.concatenate([jnp.where(at, p[k : k + 1], 0.0) for p in pieces], axis=0).astype(BF16))
        rights.append(one(iota((128, 128), 1) == lane2[:, k : k + 1]))
    got = mm(jnp.concatenate(lefts, axis=1), jnp.concatenate(rights, axis=0))
    codes = got[0:na] + 256.0 * got[na : 2 * na] + 8192.0 * got[2 * na : 3 * na] + 262144.0 * over
    gates = got[3 * na : 4 * na] + got[4 * na : 5 * na] + got[5 * na : 6 * na]
    return codes, gates


def packed(f):
    lanes = mm(f, one(iota((32, 128), 0) == (iota((32, 128), 1) & 31)))
    keep = lax.shift_right_logical(iota((16, 128), 0), 2) == lax.shift_right_logical(iota((16, 128), 1), 5)
    lanes = jnp.where(keep, lanes, 0.0)
    return lanes[0:4] + lanes[4:8] + lanes[8:12] + lanes[12:16]


def kernel(cap, feat_hbm, key_hbm, val_hbm, chosen_hbm, scores_hbm, out, flag,
           feat, chosen, scores, keys, vals, table, msg, got, fplace, idx_v, idx_s, sel_v, gate_v, picked,
           part, pair, half, zbuf, wbuf, wvec, obuf, dbuf,
           in_sem, idx_sem, a_send, a_recv, p_send, p_recv, z_send, z_recv, w_send, w_recv, d_send, d_recv, known):
    nb = cap // 128
    nh = 8 * nb
    ep, tp = lax.axis_index("ep"), lax.axis_index("tp")
    core, z = lax.rem(tp, 2), lax.div(tp, 2)
    mate = tp + 1 - 2 * core

    ins = [pltpu.make_async_copy(a, b, in_sem.at[k]) for k, (a, b) in enumerate(
        ((chosen_hbm, chosen), (scores_hbm, scores), (feat_hbm, feat), (key_hbm, keys), (val_hbm, vals)))]
    for c in ins:
        c.start()

    def along(d):
        return (ep, lax.rem(tp + 2 * d + 32, 32))

    def tell(sem, d):
        pl.semaphore_signal(sem, inc=1, device_id=along(d), device_id_type=MESH)
        pl.semaphore_signal(sem, inc=1, device_id=along(-d), device_id_type=MESH)

    barrier = pltpu.get_barrier_semaphore()
    for p in range(15, 0, -1):
        pl.semaphore_signal(barrier, inc=1, device_id=(other(ep, ORDER[p]), tp), device_id_type=MESH)
    tell(barrier, 1)
    pl.semaphore_signal(barrier, inc=1, device_id=(ep, mate), device_id_type=MESH)

    for c in ins[:3]:
        c.wait()
    codes, gates = compact(chosen[...], scores[...], cap)
    tokens = packed(feat[...])
    for e in range(16):
        msg[e, 0:nb] = codes[e * nb : (e + 1) * nb]
        msg[e, nb : 2 * nb] = gates[e * nb : (e + 1) * nb]
        msg[e, 2 * nb : 2 * nb + 4] = tokens

    def list_copy(p):
        e = other(ep, BACK[p])
        return pltpu.make_async_remote_copy(
            src_ref=msg.at[e], dst_ref=got.at[p % 2, p // 2], send_sem=a_send.at[p], recv_sem=a_recv.at[p],
            device_id=(e, tp), device_id_type=MESH)

    pl.semaphore_wait(barrier, 18)
    for p in range(15, 0, -1):
        list_copy(p).start()
    tell(known.at[0], 1)
    got[0, 0] = msg[ep]
    ins[3].wait()
    ins[4].wait()

    same = one(iota((128, 128), 0) == iota((128, 128), 1))

    def turn(b, _):
        for j in range(4):
            at = pl.multiple_of(b * 512 + j * 128, 128)
            block = jnp.concatenate(
                [keys[:, pl.ds(at, 128)], vals[:, pl.ds(at, 128)],
                 keys[:, pl.ds(at + 8192, 128)], vals[:, pl.ds(at + 8192, 128)]], axis=0)
            table[pl.ds(at, 128), :] = lax.dot_general(
                same, block, (((1,), (1,)), ((), ())), preferred_element_type=F32)
        return 0

    lax.fori_loop(0, 16, turn, 0)
    pl.semaphore_wait(known.at[0], 2)
    tell(known.at[1], 2)

    r2, c2 = iota((128, 256), 0), iota((128, 256), 1)
    fold = one((c2 & 127) - 64 * lax.shift_right_logical(c2, 7) == (r2 & 31))
    keep = lax.shift_right_logical(iota((16, 128), 0), 2) == lax.shift_right_logical(iota((16, 128), 1), 5)

    def idx_copy(h, r):
        row = h * nh + r
        return pltpu.make_async_copy(idx_v.at[h, r], idx_s.at[pl.ds(row * 128, 128)], idx_sem.at[row])

    def arrive(slots):
        for h, m in slots:
            if not (m == 0 and isinstance(h, int) and h == 0):
                pltpu.make_async_remote_copy(
                    src_ref=msg.at[0], dst_ref=got.at[h, m], send_sem=a_send.at[0], recv_sem=a_recv.at[2 * m + h],
                    device_id=(ep, mate), device_id_type=MESH).wait_recv()
        for h, m in slots:
            at = slice(m * nb, (m + 1) * nb)
            code = got[h, m, 0:nb].astype(I32)
            idx_v[h, at] = code & 8191
            sel_v[h, at] = lax.shift_right_logical(code, 13) & 31
            gate_v[h, at] = got[h, m, nb : 2 * nb]
        for h, m in slots:
            f = got[h, m, 2 * nb : 2 * nb + 4]
            f = jnp.where(keep, jnp.concatenate([f, f, f, f], axis=0), 0.0).astype(BF16)
            f = mm(f, fold).astype(BF16)
            fplace[h, m, 0:16] = f[:, 0:128]
            fplace[h, m, 16:32] = f[:, 128:256]
        for h, m in slots:
            for j in range(nb):
                idx_copy(h, m * nb + j).start()

    def fetch(slots, runs):
        for h, m in slots:
            for j in range(nb):
                idx_copy(h, m * nb + j).wait()
        for h, m, n in runs:
            first = (h * 8 + m) * cap

            def gather(g, _):
                base = pl.multiple_of(first + g * 16, 16)
                for j in range(16):
                    r = idx_s[base + j] & 8191
                    picked[pl.ds(base + j, 1), :] = table[pl.ds(r, 1), :]
                return 0

            lax.fori_loop(0, n * cap // 16, gather, 0)
        for h, m in slots:
            for j in range(nb):
                r = m * nb + j
                rows_q = picked[pl.ds(pl.multiple_of((h * nh + r) * 128, 128), 128), :].astype(BF16)
                all_q = lax.dot_general(fplace[h, m], rows_q, (((1,), (1,)), ((), ())), preferred_element_type=F32)
                mine = iota((32, 128), 0) == sel_v[h, r : r + 1]
                part[h, r : r + 1] = jnp.sum(jnp.where(mine, all_q, 0.0), axis=0, keepdims=True)

    g0 = [(0, 0), (1, 0), (0, 1), (1, 1)]
    g1 = [(0, 2), (1, 2), (0, 3), (1, 3)]
    g2 = [(1 - core, m) for m in range(4, 8)]
    g3 = [(core, m) for m in range(4, 8)]
    arrive(g0)
    arrive(g1)
    pl.semaphore_wait(known.at[1], 2)
    tell(known.at[2], 4)
    fetch(g0, [(0, 0, 2), (1, 0, 2)])
    arrive(g2)
    fetch(g1, [(0, 2, 2), (1, 2, 2)])
    arrive(g3)
    fetch(g2, [(1 - core, 4, 4)])
    pair_copy = pltpu.make_async_remote_copy(
        src_ref=part.at[1 - core], dst_ref=pair, send_sem=p_send, recv_sem=p_recv,
        device_id=(ep, mate), device_id_type=MESH)
    pair_copy.start()
    fetch(g3, [(core, 4, 4)])
    pl.semaphore_wait(known.at[2], 2)
    pair_copy.wait_recv()
    half[...] = (part[core] + pair[...]).astype(BF16)

    def z_copy(d):
        return pltpu.make_async_remote_copy(
            src_ref=half, dst_ref=zbuf.at[z], send_sem=z_send.at[d], recv_sem=z_recv.at[d],
            device_id=along(d), device_id_type=MESH)

    for d in RING:
        z_copy(d).start()
    zbuf[z] = half[...]
    worst = got[0, 0, 0:nb]
    for p in range(1, 16):
        worst = jnp.maximum(worst, got[p % 2, p // 2, 0:nb])
    flag[0, 0] = lax.shift_right_logical(jnp.max(worst).astype(I32), 18)
    for d in RING:
        z_copy(d).wait_recv()
    whole = zbuf[0].astype(F32)
    for k in range(1, 16):
        whole = whole + zbuf[k].astype(F32)
    weights = (gate_v[core] * gelu(whole)).astype(BF16)
    wbuf[core] = weights
    wvec[core] = weights.astype(F32)
    w_copy = pltpu.make_async_remote_copy(
        src_ref=wbuf.at[core], dst_ref=wbuf.at[core], send_sem=w_send, recv_sem=w_recv,
        device_id=(ep, mate), device_id_type=MESH)
    w_copy.start()

    group = lax.shift_right_logical(iota((4, 128), 1), 5)

    def sums(h):
        for m in range(8):
            acc = None
            for j in range(nb):
                r = m * nb + j
                mine = iota((32, 128), 0) == sel_v[h, r : r + 1]
                spread = jnp.where(mine, wvec[h, r : r + 1], 0.0).astype(BF16)
                rows_q = picked[pl.ds(pl.multiple_of((h * nh + r) * 128, 128), 128), :].astype(BF16)
                term = mm(spread, rows_q)
                acc = term if acc is None else acc + term
            block = acc[0:16] + pltpu.roll(acc[16:32], 64, 1)
            top, low = block[0:8], block[8:16]
            obuf[2 * m + h] = jnp.where(
                group == 0, pltpu.roll(top, 96, 1)[0:4],
                jnp.where(group == 1, top[4:8],
                          jnp.where(group == 2, pltpu.roll(low, 32, 1)[0:4], pltpu.roll(low, 64, 1)[4:8])))

    def out_copy(h, m):
        p = 2 * m + h
        y = ORDER[2 * m] // 4 + h * (ORDER[2 * m + 1] // 4 - ORDER[2 * m] // 4)
        x = ORDER[2 * m] % 4 + h * (ORDER[2 * m + 1] % 4 - ORDER[2 * m] % 4)
        s = lax.rem(lax.div(ep, 4) + y, 4) * 4 + lax.rem(lax.rem(ep, 4) + x, 4)
        return pltpu.make_async_remote_copy(
            src_ref=obuf.at[p], dst_ref=dbuf.at[p], send_sem=d_send.at[p], recv_sem=d_recv.at[p],
            device_id=(s, tp), device_id_type=MESH)

    sums(core)
    for m in range(7, 0, -1):
        out_copy(core, m).start()
    w_copy.wait_recv()
    wvec[1 - core] = wbuf[1 - core].astype(F32)
    sums(1 - core)
    for m in range(7, 0, -1):
        out_copy(1 - core, m).start()
    out_copy(1, 0).start()
    dbuf[0] = obuf[0]
    for p in range(1, 16):
        out_copy(p % 2, p // 2).wait_recv()
    full = dbuf[0]
    for p in range(1, 16):
        full = full + dbuf[p]
    full = jnp.concatenate([full, full], axis=0)
    out[...] = jnp.concatenate(
        [(pltpu.roll(full, 128 - 32 * j, 1) if j else full)[0:4, 0:32] for j in range(4)], axis=0).astype(BF16)

    for p in range(1, 16):
        list_copy(p).wait_send()
        z_copy(p).wait_send()
        out_copy(p % 2, p // 2).wait_send()
    pair_copy.wait_send()
    w_copy.wait_send()


def run(cap, cid, feat, key_t, val_t, chosen, scores):
    nb = cap // 128
    nh = 8 * nb
    dma = pltpu.SemaphoreType.DMA
    vmem = pltpu.VMEM
    return pl.pallas_call(
        functools.partial(kernel, cap),
        out_shape=(jax.ShapeDtypeStruct((16, 32), BF16), jax.ShapeDtypeStruct((1, 1), I32)),
        in_specs=[pl.BlockSpec(memory_space=pl.ANY)] * 5,
        out_specs=(pl.BlockSpec(memory_space=vmem), pl.BlockSpec(memory_space=pltpu.SMEM)),
        scratch_shapes=[
            vmem((16, 32), BF16), vmem((64, 16), I32), vmem((64, 16), F32), vmem((32, 16384), BF16), vmem((32, 16384), BF16),
            vmem((8192, 128), F32), vmem((16, 2 * nb + 4, 128), F32), vmem((2, 8, 2 * nb + 4, 128), F32),
            vmem((2, 8, 32, 128), BF16), vmem((2, nh, 128), I32), pltpu.SMEM((2 * nh * 128,), I32),
            vmem((2, nh, 128), I32), vmem((2, nh, 128), F32), vmem((2 * nh * 128, 128), F32),
            vmem((2, nh, 128), F32), vmem((nh, 128), F32), vmem((nh, 128), BF16), vmem((16, nh, 128), BF16),
            vmem((2, nh, 128), BF16), vmem((2, nh, 128), F32), vmem((16, 4, 128), F32), vmem((16, 4, 128), F32),
            dma((5,)), dma((2 * nh,)), dma((16,)), dma((16,)), dma, dma, dma((16,)), dma((16,)), dma, dma,
            dma((16,)), dma((16,)), pltpu.SemaphoreType.REGULAR((3,)),
        ],
        compiler_params=pltpu.CompilerParams(collective_id=cid, has_side_effects=True, vmem_limit_bytes=48 << 20),
    )(feat, key_t, val_t, chosen, scores)


def blocks(func, arrays):
    split = tuple(x.reshape((8, 32) + x.shape[1:]) for x in arrays)
    done = lax.map(func, split)
    return done.reshape((256,) + done.shape[2:])


def dense(features, key_table, value_table, chosen, scores):
    first = lax.axis_index("ep") * 16384
    every = lax.all_gather(chosen, "ep", axis=0, tiled=True)
    gates = lax.all_gather(jax.nn.softmax(scores, axis=-1), "ep", axis=0, tiled=True).reshape(256, 64)
    tokens = lax.all_gather(features, "ep", axis=0, tiled=True)
    shifted = every.reshape(256, 64) - first
    owned = (shifted >= 0) & (shifted < 16384)
    rows = jnp.clip(shifted, 0, 16383)

    def dots(pair):
        block, at = pair
        full = lax.dot_general(block, key_table, (((1,), (1,)), ((), ())), preferred_element_type=F32)
        return jnp.take_along_axis(full, at, axis=1)

    partial = jnp.where(owned, blocks(dots, (tokens, rows)), 0.0)
    products = jnp.concatenate(
        [lax.all_gather(partial[k * 64 : (k + 1) * 64], "tp").sum(0) for k in range(4)], axis=0)
    weights = (gates * jax.nn.gelu(products, approximate=False)).astype(BF16)
    weights = jnp.where(owned, weights, jnp.zeros_like(weights))

    def spread(pair):
        block, at = pair
        ids = lax.broadcasted_iota(I32, at.shape, 0)
        full = jnp.zeros((32, 16384), F32).at[ids, at].add(block.astype(F32))
        upper = full.astype(BF16)
        lower = (full - upper.astype(F32)).astype(BF16)
        return mm(upper, value_table) + mm(lower, value_table)

    terms = lax.all_gather(blocks(spread, (weights, rows)), "ep").sum(0)
    return lax.dynamic_slice_in_dim(terms, lax.axis_index("ep") * 16, 16, 0).astype(BF16)


def local(features, key_table, value_table, chosen, scores):
    quick, flag = run(256, 0, features, key_table.T, value_table.T, chosen.reshape(64, 16), scores.reshape(64, 16))
    return lax.cond(flag[0, 0] > 0, lambda: dense(features, key_table, value_table, chosen, scores), lambda: quick)


def solution(mesh):
    spec = P("ep", "tp")
    whole = P("ep", None, None)
    return jax.shard_map(local, mesh=mesh, in_specs=(spec, spec, spec, whole, whole), out_specs=spec, check_vma=False)
```

```python
import functools

import jax
import jax.numpy as jnp
from jax import lax
from jax.experimental import pallas as pl
from jax.experimental.pallas import tpu as pltpu
from jax.sharding import PartitionSpec as P

MESH = pl.DeviceIdType.MESH
F32 = jnp.float32
BF16 = jnp.bfloat16
I32 = jnp.int32


def hops(d):
    return min(d // 4, 4 - d // 4) + min(d % 4, 4 - d % 4)


ORDER = sorted(range(16), key=hops)
BACK = [(-(d // 4)) % 4 * 4 + (-(d % 4)) % 4 for d in ORDER]
RING = sorted(range(1, 16), key=lambda d: -min(d, 16 - d))


def other(ep, d):
    y, x = lax.div(ep, 4), lax.rem(ep, 4)
    return lax.rem(y + d // 4, 4) * 4 + lax.rem(x + d % 4, 4)


def iota(shape, dim):
    return lax.broadcasted_iota(I32, shape, dim)


def one(cond):
    return jnp.where(cond, 1.0, 0.0).astype(BF16)


def mm(a, b):
    return jnp.dot(a, b, preferred_element_type=F32)


def gelu(x):
    return 0.5 * x * (1.0 + lax.erf(x * (2.0 ** -0.5)))


def compact(ch, sc, cap):
    nb = cap // 128
    na = 16 * nb
    own = lax.shift_right_logical(ch, 14)
    row = ch & 16383
    rep = one((iota((16, 256), 1) & 15) == iota((16, 256), 0))
    ownrep = mm(own.astype(F32).astype(BF16), rep)
    hit = ownrep == lax.shift_right_logical(iota((64, 256), 1), 4).astype(F32)
    hits = one(hit)
    before = mm(one(iota((64, 64), 1) < iota((64, 64), 0)), hits)
    total = mm(jnp.ones((8, 64), BF16), hits)
    r2, c2 = iota((256, 256), 0), iota((256, 256), 1)
    step = one((lax.shift_right_logical(r2, 4) == lax.shift_right_logical(c2, 4)) & ((r2 & 15) < (c2 & 15)))
    start = mm(total.astype(BF16), step)
    over = jnp.max(jnp.where(start + total > float(cap), 1.0, 0.0), axis=1, keepdims=True)[0:1]
    place = jnp.where(hit, before + start[0:1], 0.0).astype(I32)
    fold = one((iota((256, 16), 0) & 15) == iota((256, 16), 1))
    low = mm((place & 255).astype(F32).astype(BF16), fold)
    high = mm(lax.shift_right_logical(place, 8).astype(F32).astype(BF16), fold)
    rank = (low + 256.0 * high).astype(I32)
    line = own * nb + lax.shift_right_logical(rank, 7)
    line = jnp.where(rank < cap, line, -1)
    lane = rank & 127
    top = jnp.max(sc, axis=1, keepdims=True)
    ex = jnp.exp(sc - top)
    gate = ex / jnp.sum(ex, axis=1, keepdims=True)
    wide = jnp.concatenate(
        [line.astype(F32), row.astype(F32), gate, jnp.zeros((64, 80), F32)], axis=1)
    wide = jnp.concatenate([wide, jnp.zeros((64, 128), F32)], axis=0)
    turned = wide.T

    def two(x):
        return jnp.concatenate([x[0:8, 0:64], x[8:16, 0:64]], axis=1)

    line_t = two(turned[0:16]).astype(I32)
    row_t = two(turned[16:32]).astype(I32)
    gate_t = two(turned[32:48])
    g1 = gate_t.astype(BF16).astype(F32)
    g2 = (gate_t - g1).astype(BF16).astype(F32)
    g3 = gate_t - g1 - g2
    token = lax.shift_right_logical(iota((8, 128), 1) & 63, 2)
    pieces = (
        (row_t & 255).astype(F32),
        (lax.shift_right_logical(row_t, 8) & 31).astype(F32),
        (lax.shift_right_logical(row_t, 13) * 16 + token).astype(F32),
        g1, g2, g3,
    )
    lane2 = jnp.concatenate([lane[:, 0:8], lane[:, 8:16]], axis=0)
    lefts, rights = [], []
    for k in range(8):
        at = iota((na, 128), 0) == line_t[k : k + 1]
        lefts.append(jnp.concatenate([jnp.where(at, p[k : k + 1], 0.0) for p in pieces], axis=0).astype(BF16))
        rights.append(one(iota((128, 128), 1) == lane2[:, k : k + 1]))
    got = mm(jnp.concatenate(lefts, axis=1), jnp.concatenate(rights, axis=0))
    codes = got[0:na] + 256.0 * got[na : 2 * na] + 8192.0 * got[2 * na : 3 * na] + 262144.0 * over
    gates = got[3 * na : 4 * na] + got[4 * na : 5 * na] + got[5 * na : 6 * na]
    return codes, gates


def packed(f):
    lanes = mm(f, one(iota((32, 128), 0) == (iota((32, 128), 1) & 31)))
    keep = lax.shift_right_logical(iota((16, 128), 0), 2) == lax.shift_right_logical(iota((16, 128), 1), 5)
    lanes = jnp.where(keep, lanes, 0.0)
    return lanes[0:4] + lanes[4:8] + lanes[8:12] + lanes[12:16]


def kernel(cap, feat_hbm, key_hbm, val_hbm, chosen_hbm, scores_hbm, out, flag,
           feat, chosen, scores, keys, vals, table, msg, got, fplace, idx_v, idx_s, sel_v, gate_v, picked,
           part, pair, half, zbuf, wbuf, wvec, obuf, dbuf,
           in_sem, idx_sem, a_send, a_recv, p_send, p_recv, z_send, z_recv, w_send, w_recv, d_send, d_recv, known):
    nb = cap // 128
    nh = 8 * nb
    nw = nb // 2
    ep, tp = lax.axis_index("ep"), lax.axis_index("tp")
    core, z = lax.rem(tp, 2), lax.div(tp, 2)
    mate = tp + 1 - 2 * core

    ins = [pltpu.make_async_copy(a, b, in_sem.at[k]) for k, (a, b) in enumerate(
        ((chosen_hbm, chosen), (scores_hbm, scores), (feat_hbm, feat), (key_hbm, keys), (val_hbm, vals)))]
    for c in ins:
        c.start()

    def along(d):
        return (ep, lax.rem(tp + 2 * d + 32, 32))

    def tell(sem, d):
        pl.semaphore_signal(sem, inc=1, device_id=along(d), device_id_type=MESH)
        pl.semaphore_signal(sem, inc=1, device_id=along(-d), device_id_type=MESH)

    barrier = pltpu.get_barrier_semaphore()
    for p in range(15, 0, -1):
        pl.semaphore_signal(barrier, inc=1, device_id=(other(ep, ORDER[p]), tp), device_id_type=MESH)
    tell(barrier, 1)
    pl.semaphore_signal(barrier, inc=1, device_id=(ep, mate), device_id_type=MESH)

    for c in ins[:3]:
        c.wait()
    codes, gates = compact(chosen[...], scores[...], cap)
    tokens = packed(feat[...])
    for e in range(16):
        msg[e, 0:nb] = codes[e * nb : (e + 1) * nb]
        msg[e, nb : 2 * nb] = gates[e * nb : (e + 1) * nb]
        msg[e, 2 * nb : 2 * nb + 4] = tokens

    def list_copy(p):
        e = other(ep, BACK[p])
        return pltpu.make_async_remote_copy(
            src_ref=msg.at[e], dst_ref=got.at[p % 2, p // 2], send_sem=a_send.at[p], recv_sem=a_recv.at[p],
            device_id=(e, tp), device_id_type=MESH)

    pl.semaphore_wait(barrier, 18)
    for p in range(15, 0, -1):
        list_copy(p).start()
    tell(known.at[0], 1)
    got[0, 0] = msg[ep]
    ins[3].wait()
    ins[4].wait()

    same = one(iota((128, 128), 0) == iota((128, 128), 1))

    def turn(b, _):
        for j in range(4):
            at = pl.multiple_of(b * 512 + j * 128, 128)
            block = jnp.concatenate(
                [keys[:, pl.ds(at, 128)], vals[:, pl.ds(at, 128)],
                 keys[:, pl.ds(at + 8192, 128)], vals[:, pl.ds(at + 8192, 128)]], axis=0)
            table[pl.ds(at, 128), :] = lax.dot_general(
                same, block, (((1,), (1,)), ((), ())), preferred_element_type=F32)
        return 0

    lax.fori_loop(0, 16, turn, 0)
    pl.semaphore_wait(known.at[0], 2)
    tell(known.at[1], 2)

    r2, c2 = iota((128, 256), 0), iota((128, 256), 1)
    fold = one((c2 & 127) - 64 * lax.shift_right_logical(c2, 7) == (r2 & 31))
    keep = lax.shift_right_logical(iota((16, 128), 0), 2) == lax.shift_right_logical(iota((16, 128), 1), 5)

    def idx_copy(h, r):
        row = h * (nh // 2) + r
        return pltpu.make_async_copy(idx_v.at[h, r], idx_s.at[pl.ds(row * 128, 128)], idx_sem.at[row])

    def arrive(slots):
        for h, m in slots:
            if not (m == 0 and isinstance(h, int) and h == 0):
                pltpu.make_async_remote_copy(
                    src_ref=msg.at[0], dst_ref=got.at[h, m], send_sem=a_send.at[0], recv_sem=a_recv.at[2 * m + h],
                    device_id=(ep, mate), device_id_type=MESH).wait_recv()
        for h, m in slots:
            at = slice(m * nb, (m + 1) * nb)
            code = got[h, m, 0:nb].astype(I32)
            idx_v[h, m * nw : (m + 1) * nw] = (code[0:nw] & 8191) | lax.shift_left(code[nw:nb] & 8191, 19)
            sel_v[h, at] = lax.shift_right_logical(code, 13) & 31
            gate_v[h, at] = got[h, m, nb : 2 * nb]
        for h, m in slots:
            f = got[h, m, 2 * nb : 2 * nb + 4]
            f = jnp.where(keep, jnp.concatenate([f, f, f, f], axis=0), 0.0).astype(BF16)
            f = mm(f, fold).astype(BF16)
            fplace[h, m, 0:16] = f[:, 0:128]
            fplace[h, m, 16:32] = f[:, 128:256]
        for h, m in slots:
            for j in range(nw):
                idx_copy(h, m * nw + j).start()

    def fetch(slots, runs):
        for h, m in slots:
            for j in range(nw):
                idx_copy(h, m * nw + j).wait()
        for h, m, n in runs:
            first = h * 8 + m

            def list_of(k, _):
                def gather(g, _):
                    word = (first + k) * (nw * 128) + g * 16
                    base = pl.multiple_of((first + k) * cap + g * 16, 16)
                    for j in range(16):
                        w = idx_s[word + j]
                        picked[pl.ds(base + j, 1), :] = table[pl.ds(w & 8191, 1), :]
                        picked[pl.ds(base + (nw * 128 + j), 1), :] = table[pl.ds(lax.shift_right_logical(w, 19), 1), :]
                    return 0

                return lax.fori_loop(0, nw * 8, gather, 0)

            lax.fori_loop(0, n, list_of, 0)
        for h, m in slots:
            for j in range(nb):
                r = m * nb + j
                rows_q = picked[pl.ds(pl.multiple_of((h * nh + r) * 128, 128), 128), :].astype(BF16)
                all_q = lax.dot_general(fplace[h, m], rows_q, (((1,), (1,)), ((), ())), preferred_element_type=F32)
                mine = iota((32, 128), 0) == sel_v[h, r : r + 1]
                part[h, r : r + 1] = jnp.sum(jnp.where(mine, all_q, 0.0), axis=0, keepdims=True)

    g0 = [(0, 0), (1, 0), (0, 1), (1, 1)]
    g1 = [(0, 2), (1, 2), (0, 3), (1, 3)]
    g2 = [(1 - core, m) for m in range(4, 8)]
    g3 = [(core, m) for m in range(4, 8)]
    arrive(g0)
    arrive(g1)
    fetch(g0, [(0, 0, 2), (1, 0, 2)])
    pl.semaphore_wait(known.at[1], 2)
    tell(known.at[2], 4)
    arrive(g2)
    fetch(g1, [(0, 2, 2), (1, 2, 2)])
    arrive(g3)
    fetch(g2, [(1 - core, 4, 4)])
    pair_copy = pltpu.make_async_remote_copy(
        src_ref=part.at[1 - core], dst_ref=pair, send_sem=p_send, recv_sem=p_recv,
        device_id=(ep, mate), device_id_type=MESH)
    pair_copy.start()
    fetch(g3, [(core, 4, 4)])
    pl.semaphore_wait(known.at[2], 2)
    pair_copy.wait_recv()
    half[...] = (part[core] + pair[...]).astype(BF16)

    def z_copy(d):
        return pltpu.make_async_remote_copy(
            src_ref=half, dst_ref=zbuf.at[z], send_sem=z_send.at[d], recv_sem=z_recv.at[d],
            device_id=along(d), device_id_type=MESH)

    for d in RING:
        z_copy(d).start()
    zbuf[z] = half[...]
    worst = got[0, 0, 0:nb]
    for p in range(1, 16):
        worst = jnp.maximum(worst, got[p % 2, p // 2, 0:nb])
    flag[0, 0] = lax.shift_right_logical(jnp.max(worst).astype(I32), 18)
    for d in RING:
        z_copy(d).wait_recv()
    whole = zbuf[0].astype(F32)
    for k in range(1, 16):
        whole = whole + zbuf[k].astype(F32)
    weights = (gate_v[core] * gelu(whole)).astype(BF16)
    wbuf[core] = weights
    wvec[core] = weights.astype(F32)
    w_copy = pltpu.make_async_remote_copy(
        src_ref=wbuf.at[core], dst_ref=wbuf.at[core], send_sem=w_send, recv_sem=w_recv,
        device_id=(ep, mate), device_id_type=MESH)
    w_copy.start()

    group = lax.shift_right_logical(iota((4, 128), 1), 5)

    def sums(h):
        for m in range(8):
            acc = None
            for j in range(nb):
                r = m * nb + j
                mine = iota((32, 128), 0) == sel_v[h, r : r + 1]
                spread = jnp.where(mine, wvec[h, r : r + 1], 0.0).astype(BF16)
                rows_q = picked[pl.ds(pl.multiple_of((h * nh + r) * 128, 128), 128), :].astype(BF16)
                term = mm(spread, rows_q)
                acc = term if acc is None else acc + term
            block = acc[0:16] + pltpu.roll(acc[16:32], 64, 1)
            top, low = block[0:8], block[8:16]
            obuf[2 * m + h] = jnp.where(
                group == 0, pltpu.roll(top, 96, 1)[0:4],
                jnp.where(group == 1, top[4:8],
                          jnp.where(group == 2, pltpu.roll(low, 32, 1)[0:4], pltpu.roll(low, 64, 1)[4:8])))

    def out_copy(h, m):
        p = 2 * m + h
        y = ORDER[2 * m] // 4 + h * (ORDER[2 * m + 1] // 4 - ORDER[2 * m] // 4)
        x = ORDER[2 * m] % 4 + h * (ORDER[2 * m + 1] % 4 - ORDER[2 * m] % 4)
        s = lax.rem(lax.div(ep, 4) + y, 4) * 4 + lax.rem(lax.rem(ep, 4) + x, 4)
        return pltpu.make_async_remote_copy(
            src_ref=obuf.at[p], dst_ref=dbuf.at[p], send_sem=d_send.at[p], recv_sem=d_recv.at[p],
            device_id=(s, tp), device_id_type=MESH)

    sums(core)
    for m in range(7, 0, -1):
        out_copy(core, m).start()
    w_copy.wait_recv()
    wvec[1 - core] = wbuf[1 - core].astype(F32)
    sums(1 - core)
    for m in range(7, 0, -1):
        out_copy(1 - core, m).start()
    out_copy(1, 0).start()
    dbuf[0] = obuf[0]
    for p in range(1, 16):
        out_copy(p % 2, p // 2).wait_recv()
    full = dbuf[0]
    for p in range(1, 16):
        full = full + dbuf[p]
    full = jnp.concatenate([full, full], axis=0)
    out[...] = jnp.concatenate(
        [(pltpu.roll(full, 128 - 32 * j, 1) if j else full)[0:4, 0:32] for j in range(4)], axis=0).astype(BF16)

    for p in range(1, 16):
        list_copy(p).wait_send()
        z_copy(p).wait_send()
        out_copy(p % 2, p // 2).wait_send()
    pair_copy.wait_send()
    w_copy.wait_send()


def run(cap, cid, feat, key_t, val_t, chosen, scores):
    nb = cap // 128
    nh = 8 * nb
    dma = pltpu.SemaphoreType.DMA
    vmem = pltpu.VMEM
    return pl.pallas_call(
        functools.partial(kernel, cap),
        out_shape=(jax.ShapeDtypeStruct((16, 32), BF16), jax.ShapeDtypeStruct((1, 1), I32)),
        in_specs=[pl.BlockSpec(memory_space=pl.ANY)] * 5,
        out_specs=(pl.BlockSpec(memory_space=vmem), pl.BlockSpec(memory_space=pltpu.SMEM)),
        scratch_shapes=[
            vmem((16, 32), BF16), vmem((64, 16), I32), vmem((64, 16), F32), vmem((32, 16384), BF16), vmem((32, 16384), BF16),
            vmem((8192, 128), F32), vmem((16, 2 * nb + 4, 128), F32), vmem((2, 8, 2 * nb + 4, 128), F32),
            vmem((2, 8, 32, 128), BF16), vmem((2, nh // 2, 128), I32), pltpu.SMEM((nh * 128,), I32),
            vmem((2, nh, 128), I32), vmem((2, nh, 128), F32), vmem((2 * nh * 128, 128), F32),
            vmem((2, nh, 128), F32), vmem((nh, 128), F32), vmem((nh, 128), BF16), vmem((16, nh, 128), BF16),
            vmem((2, nh, 128), BF16), vmem((2, nh, 128), F32), vmem((16, 4, 128), F32), vmem((16, 4, 128), F32),
            dma((5,)), dma((nh,)), dma((16,)), dma((16,)), dma, dma, dma((16,)), dma((16,)), dma, dma,
            dma((16,)), dma((16,)), pltpu.SemaphoreType.REGULAR((3,)),
        ],
        compiler_params=pltpu.CompilerParams(collective_id=cid, has_side_effects=True, vmem_limit_bytes=48 << 20),
    )(feat, key_t, val_t, chosen, scores)


def blocks(func, arrays):
    split = tuple(x.reshape((8, 32) + x.shape[1:]) for x in arrays)
    done = lax.map(func, split)
    return done.reshape((256,) + done.shape[2:])


def dense(features, key_table, value_table, chosen, scores):
    first = lax.axis_index("ep") * 16384
    every = lax.all_gather(chosen, "ep", axis=0, tiled=True)
    gates = lax.all_gather(jax.nn.softmax(scores, axis=-1), "ep", axis=0, tiled=True).reshape(256, 64)
    tokens = lax.all_gather(features, "ep", axis=0, tiled=True)
    shifted = every.reshape(256, 64) - first
    owned = (shifted >= 0) & (shifted < 16384)
    rows = jnp.clip(shifted, 0, 16383)

    def dots(pair):
        block, at = pair
        full = lax.dot_general(block, key_table, (((1,), (1,)), ((), ())), preferred_element_type=F32)
        return jnp.take_along_axis(full, at, axis=1)

    partial = jnp.where(owned, blocks(dots, (tokens, rows)), 0.0)
    products = jnp.concatenate(
        [lax.all_gather(partial[k * 64 : (k + 1) * 64], "tp").sum(0) for k in range(4)], axis=0)
    weights = (gates * jax.nn.gelu(products, approximate=False)).astype(BF16)
    weights = jnp.where(owned, weights, jnp.zeros_like(weights))

    def spread(pair):
        block, at = pair
        ids = lax.broadcasted_iota(I32, at.shape, 0)
        full = jnp.zeros((32, 16384), F32).at[ids, at].add(block.astype(F32))
        upper = full.astype(BF16)
        lower = (full - upper.astype(F32)).astype(BF16)
        return mm(upper, value_table) + mm(lower, value_table)

    terms = lax.all_gather(blocks(spread, (weights, rows)), "ep").sum(0)
    return lax.dynamic_slice_in_dim(terms, lax.axis_index("ep") * 16, 16, 0).astype(BF16)


def local(features, key_table, value_table, chosen, scores):
    quick, flag = run(256, 0, features, key_table.T, value_table.T, chosen.reshape(64, 16), scores.reshape(64, 16))
    return lax.cond(flag[0, 0] > 0, lambda: dense(features, key_table, value_table, chosen, scores), lambda: quick)


def solution(mesh):
    spec = P("ep", "tp")
    whole = P("ep", None, None)
    return jax.shard_map(local, mesh=mesh, in_specs=(spec, spec, spec, whole, whole), out_specs=spec, check_vma=False)
```

```python
import functools

import jax
import jax.numpy as jnp
from jax import lax
from jax.experimental import pallas as pl
from jax.experimental.pallas import tpu as pltpu
from jax.sharding import PartitionSpec as P

MESH = pl.DeviceIdType.MESH
F32 = jnp.float32
BF16 = jnp.bfloat16
I32 = jnp.int32


def hops(d):
    return min(d // 4, 4 - d // 4) + min(d % 4, 4 - d % 4)


ORDER = sorted(range(16), key=hops)
BACK = [(-(d // 4)) % 4 * 4 + (-(d % 4)) % 4 for d in ORDER]
RING = sorted(range(1, 16), key=lambda d: -min(d, 16 - d))


def other(ep, d):
    y, x = lax.div(ep, 4), lax.rem(ep, 4)
    return lax.rem(y + d // 4, 4) * 4 + lax.rem(x + d % 4, 4)


def iota(shape, dim):
    return lax.broadcasted_iota(I32, shape, dim)


def one(cond):
    return jnp.where(cond, 1.0, 0.0).astype(BF16)


def mm(a, b):
    return jnp.dot(a, b, preferred_element_type=F32)


def gelu(x):
    return 0.5 * x * (1.0 + lax.erf(x * (2.0 ** -0.5)))


def compact(ch, sc, cap):
    nb = cap // 128
    na = 16 * nb
    own = lax.shift_right_logical(ch, 14)
    row = ch & 16383
    rep = one((iota((16, 256), 1) & 15) == iota((16, 256), 0))
    ownrep = mm(own.astype(F32).astype(BF16), rep)
    hit = ownrep == lax.shift_right_logical(iota((64, 256), 1), 4).astype(F32)
    hits = one(hit)
    before = mm(one(iota((64, 64), 1) < iota((64, 64), 0)), hits)
    total = mm(jnp.ones((8, 64), BF16), hits)
    r2, c2 = iota((256, 256), 0), iota((256, 256), 1)
    step = one((lax.shift_right_logical(r2, 4) == lax.shift_right_logical(c2, 4)) & ((r2 & 15) < (c2 & 15)))
    start = mm(total.astype(BF16), step)
    over = jnp.max(jnp.where(start + total > float(cap), 1.0, 0.0), axis=1, keepdims=True)[0:1]
    place = jnp.where(hit, before + start[0:1], 0.0).astype(I32)
    fold = one((iota((256, 16), 0) & 15) == iota((256, 16), 1))
    low = mm((place & 255).astype(F32).astype(BF16), fold)
    high = mm(lax.shift_right_logical(place, 8).astype(F32).astype(BF16), fold)
    rank = (low + 256.0 * high).astype(I32)
    line = own * nb + lax.shift_right_logical(rank, 7)
    line = jnp.where(rank < cap, line, -1)
    lane = rank & 127
    top = jnp.max(sc, axis=1, keepdims=True)
    ex = jnp.exp(sc - top)
    gate = ex / jnp.sum(ex, axis=1, keepdims=True)
    wide = jnp.concatenate(
        [line.astype(F32), row.astype(F32), gate, jnp.zeros((64, 80), F32)], axis=1)
    wide = jnp.concatenate([wide, jnp.zeros((64, 128), F32)], axis=0)
    turned = wide.T

    def two(x):
        return jnp.concatenate([x[0:8, 0:64], x[8:16, 0:64]], axis=1)

    line_t = two(turned[0:16]).astype(I32)
    row_t = two(turned[16:32]).astype(I32)
    gate_t = two(turned[32:48])
    g1 = gate_t.astype(BF16).astype(F32)
    g2 = (gate_t - g1).astype(BF16).astype(F32)
    g3 = gate_t - g1 - g2
    token = lax.shift_right_logical(iota((8, 128), 1) & 63, 2)
    pieces = (
        (row_t & 255).astype(F32),
        (lax.shift_right_logical(row_t, 8) & 31).astype(F32),
        (lax.shift_right_logical(row_t, 13) * 16 + token).astype(F32),
        g1, g2, g3,
    )
    lane2 = jnp.concatenate([lane[:, 0:8], lane[:, 8:16]], axis=0)
    lefts, rights = [], []
    for k in range(8):
        at = iota((na, 128), 0) == line_t[k : k + 1]
        lefts.append(jnp.concatenate([jnp.where(at, p[k : k + 1], 0.0) for p in pieces], axis=0).astype(BF16))
        rights.append(one(iota((128, 128), 1) == lane2[:, k : k + 1]))
    got = mm(jnp.concatenate(lefts, axis=1), jnp.concatenate(rights, axis=0))
    codes = got[0:na] + 256.0 * got[na : 2 * na] + 8192.0 * got[2 * na : 3 * na] + 262144.0 * over
    gates = got[3 * na : 4 * na] + got[4 * na : 5 * na] + got[5 * na : 6 * na]
    return codes, gates


def packed(f):
    lanes = mm(f, one(iota((32, 128), 0) == (iota((32, 128), 1) & 31)))
    keep = lax.shift_right_logical(iota((16, 128), 0), 2) == lax.shift_right_logical(iota((16, 128), 1), 5)
    lanes = jnp.where(keep, lanes, 0.0)
    return lanes[0:4] + lanes[4:8] + lanes[8:12] + lanes[12:16]


def kernel(cap, feat_hbm, key_hbm, val_hbm, chosen_hbm, scores_hbm, out, flag,
           feat, chosen, scores, keys, vals, table, msg, got, fplace, idx_v, idx_s, sel_v, gate_v, picked,
           part, pair, half, zbuf, wbuf, wvec, obuf, dbuf,
           in_sem, idx_sem, a_send, a_recv, p_send, p_recv, z_send, z_recv, w_send, w_recv, d_send, d_recv, known, told, flag_sem):
    nb = cap // 128
    nh = 8 * nb
    nw = nb // 2
    ep, tp = lax.axis_index("ep"), lax.axis_index("tp")
    core, z = lax.rem(tp, 2), lax.div(tp, 2)
    mate = tp + 1 - 2 * core

    ins = [pltpu.make_async_copy(a, b, in_sem.at[k]) for k, (a, b) in enumerate(
        ((chosen_hbm, chosen), (scores_hbm, scores), (feat_hbm, feat), (key_hbm, keys), (val_hbm, vals)))]
    for c in ins:
        c.start()

    def along(d):
        return (ep, lax.rem(tp + 2 * d + 32, 32))

    def tell(sem, d):
        pl.semaphore_signal(sem, inc=1, device_id=along(d), device_id_type=MESH)
        pl.semaphore_signal(sem, inc=1, device_id=along(-d), device_id_type=MESH)

    barrier = pltpu.get_barrier_semaphore()
    for p in range(15, 0, -1):
        pl.semaphore_signal(barrier, inc=1, device_id=(other(ep, ORDER[p]), tp), device_id_type=MESH)
    tell(barrier, 1)
    pl.semaphore_signal(barrier, inc=1, device_id=(ep, mate), device_id_type=MESH)

    for c in ins[:3]:
        c.wait()
    codes, gates = compact(chosen[...], scores[...], cap)
    tokens = packed(feat[...])
    for e in range(16):
        msg[e, 0:nb] = codes[e * nb : (e + 1) * nb]
        msg[e, nb : 2 * nb] = gates[e * nb : (e + 1) * nb]
        msg[e, 2 * nb : 2 * nb + 4] = tokens

    def list_copy(p):
        e = other(ep, BACK[p])
        return pltpu.make_async_remote_copy(
            src_ref=msg.at[e], dst_ref=got.at[p % 2, p // 2], send_sem=a_send.at[p], recv_sem=a_recv.at[p],
            device_id=(e, tp), device_id_type=MESH)

    pl.semaphore_wait(barrier, 18)
    for p in range(15, 0, -1):
        list_copy(p).start()
    tell(known.at[0], 1)
    got[0, 0] = msg[ep]
    ins[3].wait()
    ins[4].wait()

    same = one(iota((128, 128), 0) == iota((128, 128), 1))

    def turn(b, _):
        for j in range(4):
            at = pl.multiple_of(b * 512 + j * 128, 128)
            block = jnp.concatenate(
                [keys[:, pl.ds(at, 128)], vals[:, pl.ds(at, 128)],
                 keys[:, pl.ds(at + 8192, 128)], vals[:, pl.ds(at + 8192, 128)]], axis=0)
            table[pl.ds(at, 128), :] = lax.dot_general(
                same, block, (((1,), (1,)), ((), ())), preferred_element_type=F32)
        return 0

    lax.fori_loop(0, 16, turn, 0)
    pl.semaphore_wait(known.at[0], 2)
    tell(known.at[1], 2)

    r2, c2 = iota((128, 256), 0), iota((128, 256), 1)
    fold = one((c2 & 127) - 64 * lax.shift_right_logical(c2, 7) == (r2 & 31))
    keep = lax.shift_right_logical(iota((16, 128), 0), 2) == lax.shift_right_logical(iota((16, 128), 1), 5)

    def idx_copy(h, r):
        row = h * (nh // 2) + r
        return pltpu.make_async_copy(idx_v.at[h, r], idx_s.at[pl.ds(row * 128, 128)], idx_sem.at[row])

    def arrive(slots):
        for h, m in slots:
            if not (m == 0 and isinstance(h, int) and h == 0):
                pltpu.make_async_remote_copy(
                    src_ref=msg.at[0], dst_ref=got.at[h, m], send_sem=a_send.at[0], recv_sem=a_recv.at[2 * m + h],
                    device_id=(ep, mate), device_id_type=MESH).wait_recv()
        for h, m in slots:
            at = slice(m * nb, (m + 1) * nb)
            code = got[h, m, 0:nb].astype(I32)
            idx_v[h, m * nw : (m + 1) * nw] = (code[0:nw] & 8191) | lax.shift_left(code[nw:nb] & 8191, 19)
            sel_v[h, at] = lax.shift_right_logical(code, 13) & 31
            gate_v[h, at] = got[h, m, nb : 2 * nb]
        for h, m in slots:
            for j in range(nw):
                idx_copy(h, m * nw + j).start()
        for h, m in slots:
            f = got[h, m, 2 * nb : 2 * nb + 4]
            f = jnp.where(keep, jnp.concatenate([f, f, f, f], axis=0), 0.0).astype(BF16)
            f = mm(f, fold).astype(BF16)
            fplace[h, m, 0:16] = f[:, 0:128]
            fplace[h, m, 16:32] = f[:, 128:256]

    def fetch(slots, runs):
        for h, m in slots:
            for j in range(nw):
                idx_copy(h, m * nw + j).wait()
        for h, m, n in runs:
            first = h * 8 + m

            def list_of(k, _):
                def gather(g, _):
                    word = (first + k) * (nw * 128) + g * 16
                    base = pl.multiple_of((first + k) * cap + g * 16, 16)
                    for j in range(16):
                        w = idx_s[word + j]
                        picked[pl.ds(base + j, 1), :] = table[pl.ds(w & 8191, 1), :]
                        picked[pl.ds(base + (nw * 128 + j), 1), :] = table[pl.ds(lax.shift_right_logical(w, 19), 1), :]
                    return 0

                return lax.fori_loop(0, nw * 8, gather, 0)

            lax.fori_loop(0, n, list_of, 0)
        for h, m in slots:
            for j in range(nb):
                r = m * nb + j
                rows_q = picked[pl.ds(pl.multiple_of((h * nh + r) * 128, 128), 128), :].astype(BF16)
                all_q = lax.dot_general(fplace[h, m], rows_q, (((1,), (1,)), ((), ())), preferred_element_type=F32)
                mine = iota((32, 128), 0) == sel_v[h, r : r + 1]
                part[h, r : r + 1] = jnp.sum(jnp.where(mine, all_q, 0.0), axis=0, keepdims=True)

    g0 = [(0, 0), (1, 0), (0, 1), (1, 1)]
    g1 = [(0, 2), (1, 2), (0, 3), (1, 3)]
    g2 = [(1 - core, m) for m in range(4, 8)]
    g3 = [(core, m) for m in range(4, 8)]
    arrive(g0)
    arrive(g1)
    fetch(g0, [(0, 0, 2), (1, 0, 2)])
    pl.semaphore_wait(known.at[1], 2)
    tell(known.at[2], 4)
    arrive(g2)
    fetch(g1, [(0, 2, 2), (1, 2, 2)])
    arrive(g3)
    fetch(g2, [(1 - core, 4, 4)])
    pair_copy = pltpu.make_async_remote_copy(
        src_ref=part.at[1 - core], dst_ref=pair, send_sem=p_send, recv_sem=p_recv,
        device_id=(ep, mate), device_id_type=MESH)
    pair_copy.start()
    fetch(g3, [(core, 4, 4)])
    pl.semaphore_wait(known.at[2], 2)
    pair_copy.wait_recv()
    half[...] = (part[core] + pair[...]).astype(BF16)

    def z_copy(d):
        return pltpu.make_async_remote_copy(
            src_ref=half, dst_ref=zbuf.at[z], send_sem=z_send.at[d], recv_sem=z_recv.at[d],
            device_id=along(d), device_id_type=MESH)

    for d in RING:
        z_copy(d).start()
    zbuf[z] = half[...]
    worst = got[0, 0, 0:nb]
    for p in range(1, 16):
        worst = jnp.maximum(worst, got[p % 2, p // 2, 0:nb])
    told[0, 0] = lax.shift_right_logical(jnp.max(worst).astype(I32), 18)
    flag_copy = pltpu.make_async_copy(told, flag, flag_sem)
    flag_copy.start()
    for d in RING:
        z_copy(d).wait_recv()
    whole = zbuf[0].astype(F32)
    for k in range(1, 16):
        whole = whole + zbuf[k].astype(F32)
    weights = (gate_v[core] * gelu(whole)).astype(BF16)
    wbuf[core] = weights
    wvec[core] = weights.astype(F32)
    w_copy = pltpu.make_async_remote_copy(
        src_ref=wbuf.at[core], dst_ref=wbuf.at[core], send_sem=w_send, recv_sem=w_recv,
        device_id=(ep, mate), device_id_type=MESH)
    w_copy.start()

    group = lax.shift_right_logical(iota((4, 128), 1), 5)

    def sums(h):
        for m in range(8):
            acc = None
            for j in range(nb):
                r = m * nb + j
                mine = iota((32, 128), 0) == sel_v[h, r : r + 1]
                spread = jnp.where(mine, wvec[h, r : r + 1], 0.0).astype(BF16)
                rows_q = picked[pl.ds(pl.multiple_of((h * nh + r) * 128, 128), 128), :].astype(BF16)
                term = mm(spread, rows_q)
                acc = term if acc is None else acc + term
            block = acc[0:16] + pltpu.roll(acc[16:32], 64, 1)
            top, low = block[0:8], block[8:16]
            obuf[2 * m + h] = jnp.where(
                group == 0, pltpu.roll(top, 96, 1)[0:4],
                jnp.where(group == 1, top[4:8],
                          jnp.where(group == 2, pltpu.roll(low, 32, 1)[0:4], pltpu.roll(low, 64, 1)[4:8])))

    def out_copy(h, m):
        p = 2 * m + h
        y = ORDER[2 * m] // 4 + h * (ORDER[2 * m + 1] // 4 - ORDER[2 * m] // 4)
        x = ORDER[2 * m] % 4 + h * (ORDER[2 * m + 1] % 4 - ORDER[2 * m] % 4)
        s = lax.rem(lax.div(ep, 4) + y, 4) * 4 + lax.rem(lax.rem(ep, 4) + x, 4)
        return pltpu.make_async_remote_copy(
            src_ref=obuf.at[p], dst_ref=dbuf.at[p], send_sem=d_send.at[p], recv_sem=d_recv.at[p],
            device_id=(s, tp), device_id_type=MESH)

    sums(core)
    for m in range(7, 0, -1):
        out_copy(core, m).start()
    w_copy.wait_recv()
    wvec[1 - core] = wbuf[1 - core].astype(F32)
    sums(1 - core)
    for m in range(7, 0, -1):
        out_copy(1 - core, m).start()
    out_copy(1, 0).start()
    dbuf[0] = obuf[0]
    for p in range(1, 16):
        out_copy(p % 2, p // 2).wait_recv()
    full = dbuf[0]
    for p in range(1, 16):
        full = full + dbuf[p]
    full = jnp.concatenate([full, full], axis=0)
    out[...] = jnp.concatenate(
        [(pltpu.roll(full, 128 - 32 * j, 1) if j else full)[0:4, 0:32] for j in range(4)], axis=0).astype(BF16)

    for p in range(1, 16):
        list_copy(p).wait_send()
        z_copy(p).wait_send()
        out_copy(p % 2, p // 2).wait_send()
    pair_copy.wait_send()
    w_copy.wait_send()
    flag_copy.wait()


def run(cap, cid, feat, key_t, val_t, chosen, scores):
    nb = cap // 128
    nh = 8 * nb
    dma = pltpu.SemaphoreType.DMA
    vmem = pltpu.VMEM
    return pl.pallas_call(
        functools.partial(kernel, cap),
        out_shape=(jax.ShapeDtypeStruct((16, 32), BF16), jax.ShapeDtypeStruct((1, 1), I32)),
        in_specs=[pl.BlockSpec(memory_space=pl.ANY)] * 5,
        out_specs=(pl.BlockSpec(memory_space=vmem), pl.BlockSpec(memory_space=pl.ANY)),
        scratch_shapes=[
            vmem((16, 32), BF16), vmem((64, 16), I32), vmem((64, 16), F32), vmem((32, 16384), BF16), vmem((32, 16384), BF16),
            vmem((8192, 128), F32), vmem((16, 2 * nb + 4, 128), F32), vmem((2, 8, 2 * nb + 4, 128), F32),
            vmem((2, 8, 32, 128), BF16), vmem((2, nh // 2, 128), I32), pltpu.SMEM((nh * 128,), I32),
            vmem((2, nh, 128), I32), vmem((2, nh, 128), F32), vmem((2 * nh * 128, 128), F32),
            vmem((2, nh, 128), F32), vmem((nh, 128), F32), vmem((nh, 128), BF16), vmem((16, nh, 128), BF16),
            vmem((2, nh, 128), BF16), vmem((2, nh, 128), F32), vmem((16, 4, 128), F32), vmem((16, 4, 128), F32),
            dma((5,)), dma((nh,)), dma((16,)), dma((16,)), dma, dma, dma((16,)), dma((16,)), dma, dma,
            dma((16,)), dma((16,)), pltpu.SemaphoreType.REGULAR((3,)), pltpu.SMEM((1, 1), I32), dma,
        ],
        compiler_params=pltpu.CompilerParams(collective_id=cid, has_side_effects=True, vmem_limit_bytes=48 << 20),
    )(feat, key_t, val_t, chosen, scores)


def blocks(func, arrays):
    split = tuple(x.reshape((8, 32) + x.shape[1:]) for x in arrays)
    done = lax.map(func, split)
    return done.reshape((256,) + done.shape[2:])


def dense(features, key_table, value_table, chosen, scores):
    first = lax.axis_index("ep") * 16384
    every = lax.all_gather(chosen, "ep", axis=0, tiled=True)
    gates = lax.all_gather(jax.nn.softmax(scores, axis=-1), "ep", axis=0, tiled=True).reshape(256, 64)
    tokens = lax.all_gather(features, "ep", axis=0, tiled=True)
    shifted = every.reshape(256, 64) - first
    owned = (shifted >= 0) & (shifted < 16384)
    rows = jnp.clip(shifted, 0, 16383)

    def dots(pair):
        block, at = pair
        full = lax.dot_general(block, key_table, (((1,), (1,)), ((), ())), preferred_element_type=F32)
        return jnp.take_along_axis(full, at, axis=1)

    partial = jnp.where(owned, blocks(dots, (tokens, rows)), 0.0)
    products = jnp.concatenate(
        [lax.all_gather(partial[k * 64 : (k + 1) * 64], "tp").sum(0) for k in range(4)], axis=0)
    weights = (gates * jax.nn.gelu(products, approximate=False)).astype(BF16)
    weights = jnp.where(owned, weights, jnp.zeros_like(weights))

    def spread(pair):
        block, at = pair
        ids = lax.broadcasted_iota(I32, at.shape, 0)
        full = jnp.zeros((32, 16384), F32).at[ids, at].add(block.astype(F32))
        upper = full.astype(BF16)
        lower = (full - upper.astype(F32)).astype(BF16)
        return mm(upper, value_table) + mm(lower, value_table)

    terms = lax.all_gather(blocks(spread, (weights, rows)), "ep").sum(0)
    return lax.dynamic_slice_in_dim(terms, lax.axis_index("ep") * 16, 16, 0).astype(BF16)


def local(features, key_table, value_table, chosen, scores):
    quick, flag = run(256, 0, features, key_table.T, value_table.T, chosen.reshape(64, 16), scores.reshape(64, 16))
    return lax.cond(flag[0, 0] > 0, lambda: dense(features, key_table, value_table, chosen, scores), lambda: quick)


def solution(mesh):
    spec = P("ep", "tp")
    whole = P("ep", None, None)
    return jax.shard_map(local, mesh=mesh, in_specs=(spec, spec, spec, whole, whole), out_specs=spec, check_vma=False)
```
